1024 devices in a mesh: kv: 128 (over z, y), tp: 8 (over x, core).
Axes of the slice: x: 4, y: 4, z: 32, core: 2. Of those that a mesh axis runs over, the one named last changes fastest.
Arguments:
- proposals: bfloat16 [256, 4, 4096], P('kv', None, 'tp'), may hold values from -6 to 6
- input_norm_gain: float32 [4096], replicated, may hold values from 0.1 to 1.9
- query_matrix: bfloat16 [4096, 2048], P(None, 'tp'), may hold values from -0.09375 to 0.09375
- forget_gate_matrix: bfloat16 [4096, 2048], P(None, 'tp'), may hold values from -0.09375 to 0.09375
- value_matrix: bfloat16 [4096, 2048], P(None, 'tp'), may hold values from -0.09375 to 0.09375
- forget_floor_channel: float32 [2048], P('tp'), may hold values from 0.02 to 0.95
- proposal_extra_decay: float32 [256, 4, 16], P('kv', None, 'tp'), may hold values from -0.7 to 0
- prior_proposal_states: float32 [256, 4, 2048, 128], P('kv', None, 'tp'), may hold values from -4 to 4
- accepted: int32 [256], P('kv'), may hold values from 1 to 4
- output_matrix: bfloat16 [2048, 4096], P('tp', 'kv'), may hold values from -0.02734375 to 0.02734375
Outputs:
- mixer_output: bfloat16 [256, 4, 4096], P('tp', None, 'kv')
- next_states: float32 [256, 4, 2048, 128], P('kv', None, 'tp')
The draws below stay inside these ranges and needn't reach their ends.
All inputs are finite; a program needn't handle non-finite values.
Results may differ from the reference program's by a relative error of at most 0.012.
Values may be sent and summed in bfloat16 or wider, within the bound.
No kernel may reach another device: no remote copies, remote signals or barrier semaphores. Data moves between devices by JAX's collectives and lax.ppermute only.
A program may use at most 32 MiB of HBM per device.

```python
import jax
import jax.numpy as jnp
from jax import lax

D = 4096
HEADS = 16
HEAD_DIM = 128
PROPOSALS = 4
SEQS = 256


def draw_proposal_extra_decay(key, part):
    first_key, second_key = jax.random.split(jax.random.fold_in(key, 7))
    hitting = jax.random.uniform(first_key, (SEQS, PROPOSALS, HEADS), jnp.float32) < 0.2
    keeping = jax.random.uniform(second_key, (SEQS, PROPOSALS, HEADS), jnp.float32, minval=0.5, maxval=0.8)
    return jnp.where(hitting, jnp.log(keeping), 0.0).astype(jnp.float32)


def plant(array, stream_key, smallest, top_value):
    shape = array.shape
    index_at = [jax.random.randint(jax.random.fold_in(stream_key, axis), (), 0, shape[axis]) for axis in range(len(shape))]
    array = array.at[tuple(index_at)].set(smallest)
    longest = shape.index(max(shape))
    index_at[longest] = (index_at[longest] + 1) % shape[longest]
    return array.at[tuple(index_at)].set(top_value)


def levels(rng, shape, pieces, low, largest):
    level = 1.0
    for axis_at, shards_of in pieces:
        draws = jax.random.uniform(jax.random.fold_in(jax.random.fold_in(rng, 6), axis_at), (shards_of,), jnp.float32, low / len(pieces), largest / len(pieces))
        level = level * jnp.repeat(jnp.exp(draws), shape[axis_at] // shards_of).reshape((-1,) + (1,) * (len(shape) - 1 - axis_at))
    return level


def scatter_about(key, shape, deviation, limit, cuts=(), held_as=jnp.bfloat16):
    values = jax.random.normal(key, shape, jnp.float32) * deviation
    if len(cuts) > 0:
        values = levels(key, shape, cuts, -0.22, 0.18) * values
    return jnp.clip(values, min=-limit, max=limit).astype(held_as)


def setup_inputs(seed: int = 0) -> dict:
    key_list = jax.random.split(jax.random.key(seed), 11)
    proposals = scatter_about(key_list[0], (SEQS, PROPOSALS, D), 1.0, 6.0, ((0, 128), (2, 8)))
    input_norm_gain = jnp.clip(1.0 + 0.18 * jax.random.normal(key_list[1], (D,), jnp.float32), 0.1, 1.9)
    query_matrix = scatter_about(key_list[2], (D, HEADS * HEAD_DIM), D ** -0.5, 0.09375, ((1, 8),))
    forget_gate_matrix = scatter_about(key_list[3], (D, HEADS * HEAD_DIM), D ** -0.5, 0.09375, ((1, 8),))
    value_matrix = scatter_about(key_list[4], (D, HEADS * HEAD_DIM), D ** -0.5, 0.09375, ((1, 8),))
    forget_floor_channel = jnp.clip(0.02 + 0.93 * jax.random.uniform(key_list[5], (HEADS * HEAD_DIM,), jnp.float32) ** levels(key_list[5], (HEADS * HEAD_DIM,), ((0, 8),), -0.2, 0.2), 0.02, 0.95)
    proposal_extra_decay = draw_proposal_extra_decay(jax.random.fold_in(key_list[10], 71), 0)
    prior_proposal_states = scatter_about(key_list[7], (SEQS, PROPOSALS, HEADS * HEAD_DIM, HEAD_DIM), 0.5, 4.0, ((0, 128), (2, 8)), jnp.float32)
    accepted = plant(jax.random.randint(key_list[8], (SEQS,), 1, PROPOSALS + 1), jax.random.fold_in(key_list[8], 1), 1, PROPOSALS).astype(jnp.int32)
    output_matrix = scatter_about(key_list[9], (HEADS * HEAD_DIM, D), (25 * HEADS * HEAD_DIM) ** -0.5, 0.02734375, ((0, 8), (1, 128)))
    return dict(proposals=proposals, input_norm_gain=input_norm_gain, query_matrix=query_matrix, forget_gate_matrix=forget_gate_matrix, value_matrix=value_matrix, forget_floor_channel=forget_floor_channel, proposal_extra_decay=proposal_extra_decay, prior_proposal_states=prior_proposal_states, accepted=accepted, output_matrix=output_matrix)


def reference(proposals, input_norm_gain, query_matrix, forget_gate_matrix, value_matrix, forget_floor_channel, proposal_extra_decay, prior_proposal_states, accepted, output_matrix):
    seq_count, prop_count, model_width = proposals.shape
    flat_rows = proposals.reshape(seq_count * prop_count, model_width).astype(jnp.float32)
    row_scale = lax.rsqrt(lax.optimization_barrier(jnp.mean(flat_rows * flat_rows, axis=1)) + 1e-06)[:, None]
    scaled = (flat_rows * input_norm_gain).astype(jnp.bfloat16)

    def project(weight):
        return (jnp.dot(scaled, weight, preferred_element_type=jnp.float32) * row_scale).astype(jnp.bfloat16)
    query_pre = project(query_matrix)
    forget_pre = project(forget_gate_matrix)
    value_pre = project(value_matrix)
    head_shape = (seq_count, prop_count, HEADS, HEAD_DIM)
    query_act = jax.nn.silu(query_pre.astype(jnp.float32)).reshape(head_shape)
    lower_part = forget_floor_channel.reshape(HEADS, HEAD_DIM)
    forget_gate = lower_part + (1.0 - lower_part) * jax.nn.sigmoid(forget_pre.astype(jnp.float32).reshape(head_shape))
    forget_gate_logs = jnp.log(forget_gate) + proposal_extra_decay[:, :, :, None]
    key_part = 1.0 - forget_gate
    values = value_pre.astype(jnp.float32).reshape(head_shape)
    picked = jnp.take_along_axis(prior_proposal_states, (accepted - 1).astype(jnp.int32)[:, None, None, None], axis=1)[:, 0]
    carried = picked.reshape(seq_count, HEADS, HEAD_DIM, HEAD_DIM)
    snapshots = []
    outputs = []
    for position in range(PROPOSALS):
        carried = jnp.exp(forget_gate_logs[:, position])[:, :, None, :] * carried + values[:, position][:, :, :, None] * key_part[:, position][:, :, None, :]
        outputs.append(jnp.einsum('shvk,shk->shv', carried, query_act[:, position]))
        snapshots.append(carried.reshape(seq_count, HEADS * HEAD_DIM, HEAD_DIM))
    mixed_rows = jnp.stack(outputs, axis=1).reshape(seq_count * prop_count, HEADS * HEAD_DIM)
    gated_rows = mixed_rows.astype(jnp.bfloat16)
    result = jnp.dot(gated_rows, output_matrix, preferred_element_type=jnp.float32).astype(jnp.bfloat16)
    return (result.reshape(seq_count, prop_count, model_width), jnp.stack(snapshots, axis=1))
```

```python
import jax
import jax.numpy as jnp
from jax import lax
from jax.experimental import pallas as pl
from jax.experimental.pallas import tpu as pltpu
from jax.sharding import Mesh
from jax.sharding import PartitionSpec as P

KV = ("zh", "zl", "y")
SLAB = ("zl", "y")
BF = jnp.bfloat16
F32 = jnp.float32
VM = pl.BlockSpec(memory_space=pltpu.VMEM)
SM = pl.BlockSpec(memory_space=pltpu.SMEM)
HBM = pl.BlockSpec(memory_space=pltpu.HBM)


def grant(mebibytes):
    return pltpu.CompilerParams(vmem_limit_bytes=mebibytes << 20)


def in_hbm(array):
    return pltpu.with_memory_space_constraint(array, pltpu.HBM)


def spread_kernel(rows_ref, weight_ref, rows_out_ref, weight_out_ref):
    seqs, props, width = rows_ref.shape
    rows = rows_ref[...].reshape(seqs * props, width)
    for copy in range(rows_out_ref.shape[0]):
        rows_out_ref[copy] = rows
    for copy in range(weight_out_ref.shape[0]):
        weight_out_ref[copy] = weight_ref[...]


def front_kernel(
    x_ref, gain_ref, floor_ref, picks_ref, extra_ref, wq_ref, wf_ref, wv_ref, prior_ref,
    out_ref, decay_ref, key_ref, value_ref, picked_ref, held_ref, sems, pick_sems,
):
    blocks, rows, width = x_ref.shape
    seqs, channels, dim = picked_ref.shape
    total = blocks * width
    heads = channels // dim
    props = rows // seqs
    weights = (wq_ref, wf_ref, wv_ref)
    copies = [
        [
            pltpu.make_async_copy(
                weight.at[pl.ds(block * width, width)], held_ref.at[at, block], sems.at[at, block]
            )
            for at, weight in enumerate(weights)
        ]
        for block in range(blocks)
    ]
    for group in copies:
        for copy in group:
            copy.start()
    picks = [
        pltpu.make_async_copy(
            prior_ref.at[seq, picks_ref[seq] - 1], picked_ref.at[seq], pick_sems.at[seq]
        )
        for seq in range(seqs)
    ]
    for copy in picks:
        copy.start()
    head_of = lax.broadcasted_iota(jnp.int32, (rows, channels), 1) // dim
    row_of = lax.broadcasted_iota(jnp.int32, (rows, channels), 0)
    extra = jnp.zeros((rows, channels), F32)
    for seq in range(seqs):
        for head in range(heads):
            for prop in range(props):
                here = (row_of == seq * props + prop) & (head_of == head)
                extra = jnp.where(here, extra_ref[seq, head, prop], extra)
    boost = jnp.exp(extra)
    square = jnp.zeros((rows, width), F32)
    scaled = []
    for block in range(blocks):
        x = x_ref[block].astype(F32)
        square = square + x * x
        scaled.append((x * gain_ref[:, block * width : (block + 1) * width]).astype(BF))
    sums = [jnp.zeros((rows, channels), F32) for _ in weights]
    for block in range(blocks):
        for at in range(len(weights)):
            copies[block][at].wait()
            sums[at] = sums[at] + jnp.dot(
                scaled[block], held_ref[at, block], preferred_element_type=F32
            )
    scale = lax.rsqrt(jnp.sum(square, axis=1, keepdims=True) / total + 1e-06)
    query_pre, forget_pre, value = ((s * scale).astype(BF).astype(F32) for s in sums)
    query = query_pre / (1.0 + jnp.exp(-query_pre))
    lower = floor_ref[...]
    forget = lower + (1.0 - lower) / (1.0 + jnp.exp(-forget_pre))
    key = 1.0 - forget
    decay = forget * boost
    decay_ref[...] = decay
    key_ref[...] = key
    value_ref[...] = value

    step = row_of % props
    carried = decay
    through = query
    mixed = jnp.zeros((rows, channels), F32)
    for lag in range(props):
        product = (key if lag == 0 else pltpu.roll(key, lag, 0)) * through
        weight = jnp.zeros((rows, channels), F32)
        for head in range(heads):
            weight = jnp.where(
                head_of == head,
                jnp.sum(product[:, head * dim : (head + 1) * dim], axis=1, keepdims=True),
                weight,
            )
        late = value if lag == 0 else pltpu.roll(value, lag, 0)
        mixed = mixed + jnp.where(step >= lag, weight * late, 0.0)
        earlier = decay if lag == 0 else pltpu.roll(decay, lag, 0)
        through = through * earlier
        if lag > 0:
            carried = jnp.where(step >= lag, carried * earlier, carried)
    reach = query * carried
    for copy in picks:
        copy.wait()
    seq_of = lax.broadcasted_iota(jnp.int32, (rows, dim), 0) // props
    for head in range(heads):
        span = slice(head * dim, (head + 1) * dim)
        old = jnp.zeros((rows, dim), F32)
        for seq in range(seqs):
            part = lax.dot_general(
                reach[:, span],
                picked_ref[seq, span, :],
                (((1,), (1,)), ((), ())),
                precision=lax.Precision.HIGHEST,
                preferred_element_type=F32,
            )
            old = jnp.where(seq_of == seq, part, old)
        gated = (mixed[:, span] + old).astype(BF)
        for copy in range(out_ref.shape[0]):
            out_ref[copy, :, span] = gated


def states_kernel(picked_ref, decay_ref, key_ref, value_ref, out_ref):
    seqs, props, channels, dim = out_ref.shape
    columns = value_ref[...].T
    for seq in range(seqs):
        for head in range(channels // dim):
            span = slice(head * dim, (head + 1) * dim)
            state = picked_ref[seq, span, :]
            for prop in range(props):
                row = seq * props + prop
                state = (
                    decay_ref[row : row + 1, span] * state
                    + columns[span, row : row + 1] * key_ref[row : row + 1, span]
                )
                out_ref[seq, prop, span, :] = state


def partial_kernel(props, features, rows_ref, weight_ref, out_ref, sums_ref):
    groups = 128 // features
    rows = rows_ref[...]
    count = rows.shape[0] // props
    lane_group = lax.broadcasted_iota(jnp.int32, (count, 128), 1) // features
    for chunk in range(sums_ref.shape[0]):
        sums_ref[chunk] = lax.dot_general(
            rows,
            weight_ref[chunk * 128 : (chunk + 1) * 128, :],
            (((1,), (1,)), ((), ())),
            preferred_element_type=F32,
        )
    for chunk in range(sums_ref.shape[0]):
        strips = [sums_ref[chunk, pl.ds(prop, count, stride=props), :] for prop in range(props)]
        for group in range(groups):
            packed = jnp.zeros((count, 128), F32)
            for prop in range(props):
                shift = (prop - group) % groups * features
                moved = strips[prop] if shift == 0 else pltpu.roll(strips[prop], shift, 1)
                packed = jnp.where(lane_group == prop, moved, packed)
            out_ref[chunk * groups + group] = packed


def per_device(
    proposals,
    input_norm_gain,
    query_matrix,
    forget_gate_matrix,
    value_matrix,
    forget_floor_channel,
    proposal_extra_decay,
    prior_proposal_states,
    accepted,
    output_matrix,
):
    seqs, props, width = proposals.shape
    rows = seqs * props
    channels = query_matrix.shape[1]
    dim = prior_proposal_states.shape[3]
    features = output_matrix.shape[1]
    tp = lax.axis_size("tp")
    planes = lax.axis_size("zh")
    slab = lax.axis_size(SLAB)
    shape = jax.ShapeDtypeStruct

    spread, weights = pl.pallas_call(
        spread_kernel,
        out_shape=(
            pltpu.VMEM((tp, rows, width), BF),
            pltpu.VMEM((slab, features, channels), BF),
        ),
        in_specs=[VM] * 2,
        out_specs=[VM] * 2,
        compiler_params=grant(4),
    )(proposals, output_matrix.T)
    whole = lax.all_to_all(spread, "tp", 0, 0, tiled=True)

    out_weight = lax.all_to_all(weights, SLAB, 0, 0, tiled=True)
    out_weight = out_weight.reshape(slab * features, channels)

    blocks = tp
    front = pl.pallas_call(
        front_kernel,
        out_shape=(shape((planes, rows, channels), BF),)
        + (shape((rows, channels), F32),) * 3
        + (shape((seqs, channels, dim), F32),),
        in_specs=[VM] * 3 + [SM] * 2 + [HBM] * 4,
        out_specs=[VM] * 5,
        scratch_shapes=[
            pltpu.VMEM((3, blocks, width, channels), BF),
            pltpu.SemaphoreType.DMA((3, blocks)),
            pltpu.SemaphoreType.DMA((seqs,)),
        ],
        compiler_params=grant(16),
        cost_estimate=pl.CostEstimate(flops=8 << 20, bytes_accessed=6 << 20, transcendentals=0),
    )
    operands = (
        whole,
        input_norm_gain.reshape(1, -1),
        forget_floor_channel.reshape(1, -1),
        accepted,
        proposal_extra_decay.transpose(0, 2, 1),
        *(in_hbm(m) for m in (query_matrix, forget_gate_matrix, value_matrix)),
        in_hbm(prior_proposal_states),
    )
    gated, decay, key, value, picked = front(*operands)
    crossed = lax.all_to_all(gated, "zh", 0, 0, tiled=True)

    states = pl.pallas_call(
        states_kernel,
        out_shape=shape((seqs, props, channels, dim), F32),
        in_specs=[VM] * 4,
        out_specs=VM,
        compiler_params=grant(8),
        cost_estimate=pl.CostEstimate(flops=8 << 20, bytes_accessed=1 << 20, transcendentals=0),
    )
    next_states = states(picked, decay, key, value)

    partial = pl.pallas_call(
        lambda *refs: partial_kernel(props, features, *refs),
        out_shape=pltpu.VMEM((slab, planes * seqs, 128), F32),
        in_specs=[VM] * 2,
        out_specs=VM,
        compiler_params=grant(8),
        scratch_shapes=[pltpu.VMEM((slab * features // 128, planes * rows, 128), F32)],
        cost_estimate=pl.CostEstimate(flops=1 << 20, bytes_accessed=1 << 18, transcendentals=0),
    )(crossed.reshape(planes * rows, channels), out_weight)

    arrived = lax.all_to_all(
        partial.reshape(slab * tp, seqs, 128), ("zl", "y", "tp"), 0, 0, tiled=True
    )
    result = jnp.sum(arrived.reshape(slab, tp, seqs, 128), axis=1).astype(BF)
    return (result.reshape(slab * seqs, props, features), next_states)


def solution(mesh):
    kv, tp = mesh.shape["kv"], mesh.shape["tp"]
    split = Mesh(mesh.devices.reshape(8, kv // 32, 4, tp), ("zh", "zl", "y", "tp"))
    placed = (
        P(KV, None, "tp"),
        P(),
        P(None, "tp"),
        P(None, "tp"),
        P(None, "tp"),
        P("tp"),
        P(KV, None, "tp"),
        P(KV, None, "tp", None),
        P(KV),
        P("tp", KV),
    )
    return jax.shard_map(
        per_device,
        mesh=split,
        in_specs=placed,
        out_specs=(P("tp", None, KV), P(KV, None, "tp", None)),
        check_vma=False,
    )
```

```python
import jax
import jax.numpy as jnp
from jax import lax
from jax.experimental import pallas as pl
from jax.experimental.pallas import tpu as pltpu
from jax.sharding import Mesh
from jax.sharding import PartitionSpec as P

KV = ("zh", "zl", "y")
SLAB = ("zl", "y")
BF = jnp.bfloat16
F32 = jnp.float32
VM = pl.BlockSpec(memory_space=pltpu.VMEM)
ZL_FIRST = 1
TP_FIRST = 1
HBM = pl.BlockSpec(memory_space=pltpu.HBM)


def exchange(pieces, axes, order):
    return lax.all_to_all(pieces, axes, 0, 0, tiled=True, axis_index_groups=[list(order)])


def led_by(count, first):
    return [first] + [at for at in range(count) if at != first]


def grant(mebibytes):
    return pltpu.CompilerParams(vmem_limit_bytes=mebibytes << 20)


def in_hbm(array):
    return pltpu.with_memory_space_constraint(array, pltpu.HBM)


def spread_kernel(rows_ref, weight_ref, out_ref, held_ref, kept_ref, sems):
    copies = [
        pltpu.make_async_copy(rows_ref, held_ref, sems.at[0]),
        pltpu.make_async_copy(weight_ref, kept_ref, sems.at[1]),
    ]
    for copy in copies:
        copy.start()
    seqs, props, width = held_ref.shape
    count = seqs * props
    features, channels = kept_ref.shape
    half = features // 2
    copies[0].wait()
    rows = held_ref[...].reshape(count, width)
    copies[1].wait()
    for copy in range(out_ref.shape[0]):
        out_ref[copy, :count] = rows
        out_ref[copy, count:, :channels] = kept_ref[:half]
        out_ref[copy, count:, channels:] = kept_ref[half:]


def contract_last(left, right):
    return lax.dot_general(left, right, (((1,), (1,)), ((), ())), preferred_element_type=F32)


def front_kernel(
    order, picks_from, extra_from, x_ref, gain_from, floor_from, wq_ref, wf_ref, wv_ref, prior_ref,
    out_ref, decay_ref, key_ref, value_ref, picked_ref,
    picks_ref, extra_ref, gain_ref, floor_ref, held_ref, small_sems, sems, pick_sems,
):
    small = [
        pltpu.make_async_copy(source, kept, small_sems.at[at])
        for at, (source, kept) in enumerate(
            (
                (picks_from, picks_ref),
                (gain_from, gain_ref),
                (extra_from, extra_ref),
                (floor_from, floor_ref),
            )
        )
    ]
    for copy in small:
        copy.start()
    seqs, channels, dim = picked_ref.shape
    rows = decay_ref.shape[0]
    blocks, _, width = x_ref.shape
    total = blocks * width
    heads = channels // dim
    props = rows // seqs
    weights = (wq_ref, wf_ref, wv_ref)
    copies = [
        [
            pltpu.make_async_copy(
                weight.at[pl.ds(order[block] * width, width)], held_ref.at[at, block], sems.at[at, block]
            )
            for at, weight in enumerate(weights)
        ]
        for block in range(blocks)
    ]
    for group in copies:
        for copy in group:
            copy.start()
    small[0].wait()
    picks = [
        pltpu.make_async_copy(
            prior_ref.at[seq, picks_ref[seq] - 1], picked_ref.at[seq], pick_sems.at[seq]
        )
        for seq in range(seqs)
    ]
    for copy in picks:
        copy.start()
    for copy in small[1:]:
        copy.wait()
    square = jnp.zeros((rows, width), F32)
    scaled = []
    for block in range(blocks):
        x = x_ref[block, :rows].astype(F32)
        square = square + x * x
        scaled.append((x * gain_ref[:, order[block] * width : (order[block] + 1) * width]).astype(BF))
    head_of = lax.broadcasted_iota(jnp.int32, (rows, channels), 1) // dim
    row_of = lax.broadcasted_iota(jnp.int32, (rows, channels), 0)
    extra = jnp.zeros((rows, channels), F32)
    for seq in range(seqs):
        for head in range(heads):
            for prop in range(props):
                here = (row_of == seq * props + prop) & (head_of == head)
                extra = jnp.where(here, extra_ref[seq, head, prop], extra)
    boost = jnp.exp(extra)
    sums = [jnp.zeros((rows, channels), F32) for _ in weights]
    for block in range(blocks):
        for at in range(len(weights)):
            copies[block][at].wait()
            sums[at] = sums[at] + jnp.dot(
                scaled[block], held_ref[at, block], preferred_element_type=F32
            )
    scale = lax.rsqrt(jnp.sum(square, axis=1, keepdims=True) / total + 1e-06)
    query_pre, forget_pre, value = ((s * scale).astype(BF).astype(F32) for s in sums)
    query = query_pre / (1.0 + jnp.exp(-query_pre))
    lower = floor_ref[...]
    forget = lower + (1.0 - lower) / (1.0 + jnp.exp(-forget_pre))
    key = 1.0 - forget
    decay = forget * boost
    decay_ref[...] = decay
    key_ref[...] = key
    value_ref[...] = value

    step = row_of % props
    carried = decay
    through = query
    mixed = jnp.zeros((rows, channels), F32)
    for lag in range(props):
        product = (key if lag == 0 else pltpu.roll(key, lag, 0)) * through
        weight = jnp.zeros((rows, channels), F32)
        for head in range(heads):
            weight = jnp.where(
                head_of == head,
                jnp.sum(product[:, head * dim : (head + 1) * dim], axis=1, keepdims=True),
                weight,
            )
        late = value if lag == 0 else pltpu.roll(value, lag, 0)
        mixed = mixed + jnp.where(step >= lag, weight * late, 0.0)
        earlier = decay if lag == 0 else pltpu.roll(decay, lag, 0)
        through = through * earlier
        if lag > 0:
            carried = jnp.where(step >= lag, carried * earlier, carried)
    reach = query * carried
    high = reach.astype(BF)
    low = (reach - high.astype(F32)).astype(BF)
    reach = jnp.concatenate([high, low], axis=0)
    for copy in picks:
        copy.wait()
    seq_of = lax.broadcasted_iota(jnp.int32, (rows, dim), 0) // props
    for head in range(heads):
        span = slice(head * dim, (head + 1) * dim)
        old = jnp.zeros((rows, dim), F32)
        for seq in range(seqs):
            state = picked_ref[seq, span, :]
            state_high = state.astype(BF)
            state_low = (state - state_high.astype(F32)).astype(BF)
            part = contract_last(reach[:, span], state_high)
            part = part[:rows] + part[rows:] + contract_last(high[:, span], state_low)
            old = jnp.where(seq_of == seq, part, old)
        gated = (mixed[:, span] + old).astype(BF)
        for copy in range(out_ref.shape[0]):
            out_ref[copy, :, span] = gated


def states_kernel(picked_ref, decay_ref, key_ref, value_ref, out_ref):
    seqs, props, channels, dim = out_ref.shape
    columns = value_ref[...].T
    for seq in range(seqs):
        for head in range(channels // dim):
            span = slice(head * dim, (head + 1) * dim)
            state = picked_ref[seq, span, :]
            for prop in range(props):
                row = seq * props + prop
                state = (
                    decay_ref[row : row + 1, span] * state
                    + columns[span, row : row + 1] * key_ref[row : row + 1, span]
                )
                out_ref[seq, prop, span, :] = state


def repeat_kernel(rows_ref, out_ref):
    for copy in range(out_ref.shape[0]):
        out_ref[copy] = rows_ref[...]


def product_kernel(order, rows, features, rows_ref, weight_ref, out_ref):
    members, blocks, _, channels = rows_ref.shape
    total = jnp.zeros((members * rows, features), F32)
    for block in range(blocks):
        left = jnp.concatenate([rows_ref[order.index(at), block] for at in range(members)], axis=0)
        right = jnp.concatenate(
            [weight_ref[block, rows:, :channels], weight_ref[block, rows:, channels:]], axis=0
        )
        total = total + contract_last(left, right)
    out_ref[...] = total.astype(BF)


def per_device(
    proposals,
    input_norm_gain,
    query_matrix,
    forget_gate_matrix,
    value_matrix,
    forget_floor_channel,
    proposal_extra_decay,
    prior_proposal_states,
    accepted,
    output_matrix,
):
    seqs, props, width = proposals.shape
    rows = seqs * props
    channels = query_matrix.shape[1]
    dim = prior_proposal_states.shape[3]
    features = output_matrix.shape[1]
    tp = lax.axis_size("tp")
    planes = lax.axis_size("zh")
    slab = lax.axis_size(SLAB)
    shape = jax.ShapeDtypeStruct
    tp_order = led_by(tp, TP_FIRST)
    zl_order = led_by(lax.axis_size("zl"), ZL_FIRST)
    side = lax.axis_size("y")
    slab_order = [zl * side + y for zl in zl_order for y in range(side)]

    pieces = pl.pallas_call(
        spread_kernel,
        out_shape=pltpu.VMEM((tp, rows + features * channels // width, width), BF),
        in_specs=[HBM] * 2,
        out_specs=VM,
        scratch_shapes=[
            pltpu.VMEM(proposals.shape, BF),
            pltpu.VMEM((features, channels), BF),
            pltpu.SemaphoreType.DMA((2,)),
        ],
        compiler_params=grant(4),
    )(in_hbm(proposals), in_hbm(output_matrix.T))
    whole = exchange(pieces, "tp", tp_order)

    blocks = tp
    front = pl.pallas_call(
        lambda *refs: front_kernel(tp_order, *refs),
        out_shape=(pltpu.VMEM((tp, rows, channels), BF),)
        + (shape((rows, channels), F32),) * 3
        + (shape((seqs, channels, dim), F32),),
        in_specs=[HBM] * 2 + [VM] + [HBM] * 6,
        out_specs=[VM] * 5,
        scratch_shapes=[
            pltpu.SMEM(accepted.shape, jnp.int32),
            pltpu.SMEM((seqs, channels // dim, props), F32),
            pltpu.VMEM((1, tp * width), F32),
            pltpu.VMEM((1, channels), F32),
            pltpu.VMEM((3, blocks, width, channels), BF),
            pltpu.SemaphoreType.DMA((4,)),
            pltpu.SemaphoreType.DMA((3, blocks)),
            pltpu.SemaphoreType.DMA((seqs,)),
        ],
        compiler_params=grant(16),
        cost_estimate=pl.CostEstimate(flops=8 << 20, bytes_accessed=6 << 20, transcendentals=0),
    )
    operands = (
        in_hbm(accepted),
        in_hbm(proposal_extra_decay.transpose(0, 2, 1)),
        whole,
        in_hbm(input_norm_gain.reshape(1, -1)),
        in_hbm(forget_floor_channel.reshape(1, -1)),
        *(in_hbm(m) for m in (query_matrix, forget_gate_matrix, value_matrix)),
        in_hbm(prior_proposal_states),
    )
    gated, decay, key, value, picked = front(*operands)
    full = exchange(gated, "tp", tp_order)
    swap = [(zh * tp + t, t * tp + zh) for zh in range(planes) for t in range(tp)]
    crossed = lax.ppermute(full, ("zh", "tp"), swap)

    states = pl.pallas_call(
        states_kernel,
        out_shape=shape((seqs, props, channels, dim), F32),
        in_specs=[VM] * 4,
        out_specs=VM,
        compiler_params=grant(8),
        cost_estimate=pl.CostEstimate(flops=8 << 20, bytes_accessed=1 << 20, transcendentals=0),
    )
    next_states = states(picked, decay, key, value)

    repeated = pl.pallas_call(
        repeat_kernel,
        out_shape=pltpu.VMEM((slab, *crossed.shape), BF),
        in_specs=[VM],
        out_specs=VM,
        compiler_params=grant(4),
    )(crossed)
    gathered = exchange(repeated, SLAB, slab_order)
    result = pl.pallas_call(
        lambda *refs: product_kernel(slab_order, rows, features, *refs),
        out_shape=shape((slab * rows, features), BF),
        in_specs=[VM] * 2,
        out_specs=VM,
        compiler_params=grant(8),
    )(gathered, whole)
    return (result.reshape(slab * seqs, props, features), next_states)


def solution(mesh):
    kv, tp = mesh.shape["kv"], mesh.shape["tp"]
    split = Mesh(mesh.devices.reshape(tp, kv // (4 * tp), 4, tp), ("zh", "zl", "y", "tp"))
    placed = (
        P(KV, None, "tp"),
        P(),
        P(None, "tp"),
        P(None, "tp"),
        P(None, "tp"),
        P("tp"),
        P(KV, None, "tp"),
        P(KV, None, "tp", None),
        P(KV),
        P("tp", KV),
    )
    return jax.shard_map(
        per_device,
        mesh=split,
        in_specs=placed,
        out_specs=(P("tp", None, KV), P(KV, None, "tp", None)),
        check_vma=False,
    )
```

```python
import jax
import jax.numpy as jnp
from jax import lax
from jax.experimental import pallas as pl
from jax.experimental.pallas import tpu as pltpu
from jax.sharding import Mesh
from jax.sharding import PartitionSpec as P

KV = ("zh", "zl", "y")
SLAB = ("zl", "y")
BF = jnp.bfloat16
F32 = jnp.float32
VM = pl.BlockSpec(memory_space=pltpu.VMEM)
ZL_FIRST = 1
TP_FIRST = 1
AHEAD = 5
HBM = pl.BlockSpec(memory_space=pltpu.HBM)


def exchange(pieces, axes, order):
    return lax.all_to_all(pieces, axes, 0, 0, tiled=True, axis_index_groups=[list(order)])


def led_by(count, first):
    return [first] + [at for at in range(count) if at != first]


def grant(mebibytes):
    return pltpu.CompilerParams(vmem_limit_bytes=mebibytes << 20)


def in_hbm(array):
    return pltpu.with_memory_space_constraint(array, pltpu.HBM)


def spread_kernel(rows_ref, weight_ref, out_ref, held_ref, kept_ref, sems):
    copies = [
        pltpu.make_async_copy(rows_ref, held_ref, sems.at[0]),
        pltpu.make_async_copy(weight_ref, kept_ref, sems.at[1]),
    ]
    for copy in copies:
        copy.start()
    seqs, props, width = held_ref.shape
    count = seqs * props
    features, channels = kept_ref.shape
    half = features // 2
    copies[0].wait()
    rows = held_ref[...].reshape(count, width)
    copies[1].wait()
    for copy in range(out_ref.shape[0]):
        out_ref[copy, :count] = rows
        out_ref[copy, count:, :channels] = kept_ref[:half]
        out_ref[copy, count:, channels:] = kept_ref[half:]


def contract_last(left, right):
    return lax.dot_general(left, right, (((1,), (1,)), ((), ())), preferred_element_type=F32)


def front_kernel(
    order, picks_from, extra_from, x_ref, gain_from, floor_from, wq_ref, wf_ref, wv_ref, prior_ref,
    out_ref, decay_ref, key_ref, value_ref, picked_ref,
    picks_ref, extra_ref, gain_ref, floor_ref, held_ref, small_sems, sems, pick_sems,
):
    small = [
        pltpu.make_async_copy(source, kept, small_sems.at[at])
        for at, (source, kept) in enumerate(
            (
                (picks_from, picks_ref),
                (gain_from, gain_ref),
                (extra_from, extra_ref),
                (floor_from, floor_ref),
            )
        )
    ]
    for copy in small:
        copy.start()
    seqs, channels, dim = picked_ref.shape
    rows = decay_ref.shape[0]
    blocks, _, width = x_ref.shape
    total = blocks * width
    heads = channels // dim
    props = rows // seqs
    weights = (wq_ref, wf_ref, wv_ref)
    copies = [
        [
            pltpu.make_async_copy(
                weight.at[pl.ds(order[block] * width, width)], held_ref.at[at, block], sems.at[at, block]
            )
            for at, weight in enumerate(weights)
        ]
        for block in range(blocks)
    ]
    for group in copies[:AHEAD]:
        for copy in group:
            copy.start(priority=1)
    small[0].wait()
    picks = [
        pltpu.make_async_copy(
            prior_ref.at[seq, picks_ref[seq] - 1], picked_ref.at[seq], pick_sems.at[seq]
        )
        for seq in range(seqs)
    ]
    for copy in picks:
        copy.start()
    for copy in small[1:]:
        copy.wait()
    square = jnp.zeros((rows, width), F32)
    scaled = []
    for block in range(blocks):
        x = x_ref[block, :rows].astype(F32)
        square = square + x * x
        scaled.append((x * gain_ref[:, order[block] * width : (order[block] + 1) * width]).astype(BF))
    head_of = lax.broadcasted_iota(jnp.int32, (rows, channels), 1) // dim
    row_of = lax.broadcasted_iota(jnp.int32, (rows, channels), 0)
    extra = jnp.zeros((rows, channels), F32)
    for seq in range(seqs):
        for head in range(heads):
            for prop in range(props):
                here = (row_of == seq * props + prop) & (head_of == head)
                extra = jnp.where(here, extra_ref[seq, head, prop], extra)
    boost = jnp.exp(extra)
    sums = [jnp.zeros((rows, channels), F32) for _ in weights]
    for block in range(blocks):
        for at in range(len(weights)):
            copies[block][at].wait()
        for copy in copies[block + AHEAD] if block + AHEAD < blocks else ():
            copy.start(priority=1)
        for at in range(len(weights)):
            sums[at] = sums[at] + jnp.dot(
                scaled[block], held_ref[at, block], preferred_element_type=F32
            )
    scale = lax.rsqrt(jnp.sum(square, axis=1, keepdims=True) / total + 1e-06)
    query_pre, forget_pre, value = ((s * scale).astype(BF).astype(F32) for s in sums)
    query = query_pre / (1.0 + jnp.exp(-query_pre))
    lower = floor_ref[...]
    forget = lower + (1.0 - lower) / (1.0 + jnp.exp(-forget_pre))
    key = 1.0 - forget
    decay = forget * boost
    decay_ref[...] = decay
    key_ref[...] = key
    value_ref[...] = value

    step = row_of % props
    carried = decay
    through = query
    mixed = jnp.zeros((rows, channels), F32)
    for lag in range(props):
        product = (key if lag == 0 else pltpu.roll(key, lag, 0)) * through
        weight = jnp.zeros((rows, channels), F32)
        for head in range(heads):
            weight = jnp.where(
                head_of == head,
                jnp.sum(product[:, head * dim : (head + 1) * dim], axis=1, keepdims=True),
                weight,
            )
        late = value if lag == 0 else pltpu.roll(value, lag, 0)
        mixed = mixed + jnp.where(step >= lag, weight * late, 0.0)
        earlier = decay if lag == 0 else pltpu.roll(decay, lag, 0)
        through = through * earlier
        if lag > 0:
            carried = jnp.where(step >= lag, carried * earlier, carried)
    reach = query * carried
    high = reach.astype(BF)
    low = (reach - high.astype(F32)).astype(BF)
    reach = jnp.concatenate([high, low], axis=0)
    for copy in picks:
        copy.wait()
    seq_of = lax.broadcasted_iota(jnp.int32, (rows, dim), 0) // props
    for head in range(heads):
        span = slice(head * dim, (head + 1) * dim)
        old = jnp.zeros((rows, dim), F32)
        for seq in range(seqs):
            state = picked_ref[seq, span, :]
            state_high = state.astype(BF)
            state_low = (state - state_high.astype(F32)).astype(BF)
            part = contract_last(reach[:, span], state_high)
            part = part[:rows] + part[rows:] + contract_last(high[:, span], state_low)
            old = jnp.where(seq_of == seq, part, old)
        gated = (mixed[:, span] + old).astype(BF)
        for copy in range(out_ref.shape[0]):
            out_ref[copy, :, span] = gated


def states_kernel(picked_ref, decay_ref, key_ref, value_ref, out_ref):
    seqs, props, channels, dim = out_ref.shape
    columns = value_ref[...].T
    for seq in range(seqs):
        for head in range(channels // dim):
            span = slice(head * dim, (head + 1) * dim)
            state = picked_ref[seq, span, :]
            for prop in range(props):
                row = seq * props + prop
                state = (
                    decay_ref[row : row + 1, span] * state
                    + columns[span, row : row + 1] * key_ref[row : row + 1, span]
                )
                out_ref[seq, prop, span, :] = state


def repeat_kernel(rows_ref, out_ref):
    for copy in range(out_ref.shape[0]):
        out_ref[copy] = rows_ref[...]


def product_kernel(order, rows, features, rows_ref, weight_ref, out_ref):
    members, blocks, _, channels = rows_ref.shape
    half = features // 2
    total = jnp.zeros((members * rows, features), F32)
    for block in range(blocks):
        left = jnp.concatenate([rows_ref[order.index(at), block] for at in range(members)], axis=0)
        right = jnp.concatenate(
            [weight_ref[block, rows:, :channels], weight_ref[block, rows:, channels:]], axis=0
        )
        total = total + contract_last(left, right)
    planes = lax.axis_size("zh")
    far = (lax.axis_index("tp") + planes - lax.axis_index("zh")) % planes == planes // 2
    half = members * rows // 2
    out_ref[...] = jnp.where(
        far, jnp.concatenate([total[half:], total[:half]], axis=0), total
    ).astype(BF)


def per_device(
    proposals,
    input_norm_gain,
    query_matrix,
    forget_gate_matrix,
    value_matrix,
    forget_floor_channel,
    proposal_extra_decay,
    prior_proposal_states,
    accepted,
    output_matrix,
):
    seqs, props, width = proposals.shape
    rows = seqs * props
    channels = query_matrix.shape[1]
    dim = prior_proposal_states.shape[3]
    features = output_matrix.shape[1]
    tp = lax.axis_size("tp")
    planes = lax.axis_size("zh")
    slab = lax.axis_size(SLAB)
    shape = jax.ShapeDtypeStruct
    tp_order = led_by(tp, TP_FIRST)
    zl_order = led_by(lax.axis_size("zl"), ZL_FIRST)
    side = lax.axis_size("y")
    slab_order = [zl * side + y for zl in zl_order for y in range(side)]

    pieces = pl.pallas_call(
        spread_kernel,
        out_shape=pltpu.VMEM((tp, rows + features * channels // width, width), BF),
        in_specs=[HBM] * 2,
        out_specs=VM,
        scratch_shapes=[
            pltpu.VMEM(proposals.shape, BF),
            pltpu.VMEM((features, channels), BF),
            pltpu.SemaphoreType.DMA((2,)),
        ],
        compiler_params=grant(4),
    )(in_hbm(proposals), in_hbm(output_matrix.T))
    whole = exchange(pieces, "tp", tp_order)

    blocks = tp
    front = pl.pallas_call(
        lambda *refs: front_kernel(tp_order, *refs),
        out_shape=(pltpu.VMEM((tp, rows, channels), BF),)
        + (shape((rows, channels), F32),) * 3
        + (shape((seqs, channels, dim), F32),),
        in_specs=[HBM] * 2 + [VM] + [HBM] * 6,
        out_specs=[VM] * 5,
        scratch_shapes=[
            pltpu.SMEM(accepted.shape, jnp.int32),
            pltpu.SMEM((seqs, channels // dim, props), F32),
            pltpu.VMEM((1, tp * width), F32),
            pltpu.VMEM((1, channels), F32),
            pltpu.VMEM((3, blocks, width, channels), BF),
            pltpu.SemaphoreType.DMA((4,)),
            pltpu.SemaphoreType.DMA((3, blocks)),
            pltpu.SemaphoreType.DMA((seqs,)),
        ],
        compiler_params=grant(16),
        cost_estimate=pl.CostEstimate(flops=8 << 20, bytes_accessed=6 << 20, transcendentals=0),
    )
    operands = (
        in_hbm(accepted),
        in_hbm(proposal_extra_decay.transpose(0, 2, 1)),
        whole,
        in_hbm(input_norm_gain.reshape(1, -1)),
        in_hbm(forget_floor_channel.reshape(1, -1)),
        *(in_hbm(m) for m in (query_matrix, forget_gate_matrix, value_matrix)),
        in_hbm(prior_proposal_states),
    )
    gated, decay, key, value, picked = front(*operands)
    full = exchange(gated, "tp", tp_order)
    depth = len(zl_order)

    def index(zh, zl, t):
        return (zh * depth + zl) * tp + t

    swap = []
    for zh in range(planes):
        for t in range(tp):
            turn = depth // 2 if (t - zh) % planes == planes // 2 else 0
            for zl in range(depth):
                swap.append((index(zh, zl, t), index(t, (zl + turn) % depth, zh)))
    crossed = lax.ppermute(full, ("zh", "zl", "tp"), swap)

    states = pl.pallas_call(
        states_kernel,
        out_shape=shape((seqs, props, channels, dim), F32),
        in_specs=[VM] * 4,
        out_specs=VM,
        compiler_params=grant(8),
        cost_estimate=pl.CostEstimate(flops=8 << 20, bytes_accessed=1 << 20, transcendentals=0),
    )
    next_states = states(picked, decay, key, value)

    repeated = pl.pallas_call(
        repeat_kernel,
        out_shape=pltpu.VMEM((slab, *crossed.shape), BF),
        in_specs=[VM],
        out_specs=VM,
        compiler_params=grant(4),
    )(crossed)
    gathered = exchange(repeated, SLAB, slab_order)
    result = pl.pallas_call(
        lambda *refs: product_kernel(slab_order, rows, features, *refs),
        out_shape=shape((slab * rows, features), BF),
        in_specs=[VM] * 2,
        out_specs=VM,
        compiler_params=grant(8),
    )(gathered, whole)
    return (result.reshape(slab * seqs, props, features), next_states)


def solution(mesh):
    kv, tp = mesh.shape["kv"], mesh.shape["tp"]
    split = Mesh(mesh.devices.reshape(tp, kv // (4 * tp), 4, tp), ("zh", "zl", "y", "tp"))
    placed = (
        P(KV, None, "tp"),
        P(),
        P(None, "tp"),
        P(None, "tp"),
        P(None, "tp"),
        P("tp"),
        P(KV, None, "tp"),
        P(KV, None, "tp", None),
        P(KV),
        P("tp", KV),
    )
    return jax.shard_map(
        per_device,
        mesh=split,
        in_specs=placed,
        out_specs=(P("tp", None, KV), P(KV, None, "tp", None)),
        check_vma=False,
    )
```

```python
import jax
import jax.numpy as jnp
from jax import lax
from jax.experimental import pallas as pl
from jax.experimental.pallas import tpu as pltpu
from jax.sharding import Mesh
from jax.sharding import PartitionSpec as P

KV = ("zh", "zl", "y")
SLAB = ("zl", "y")
BF = jnp.bfloat16
F32 = jnp.float32
VM = pl.BlockSpec(memory_space=pltpu.VMEM)
ZL_FIRST = 1
Y_FIRST = 0
TP_FIRST = 5
AHEAD = 5
HBM = pl.BlockSpec(memory_space=pltpu.HBM)


def exchange(pieces, axes, order):
    return lax.all_to_all(pieces, axes, 0, 0, tiled=True, axis_index_groups=[list(order)])


def led_by(count, first):
    return [first] + [at for at in range(count) if at != first]


def grant(mebibytes):
    return pltpu.CompilerParams(vmem_limit_bytes=mebibytes << 20)


def in_hbm(array):
    return pltpu.with_memory_space_constraint(array, pltpu.HBM)


def spread_kernel(rows_ref, weight_ref, out_ref, held_ref, kept_ref, sems):
    copies = [
        pltpu.make_async_copy(rows_ref, held_ref, sems.at[0]),
        pltpu.make_async_copy(weight_ref, kept_ref, sems.at[1]),
    ]
    for copy in copies:
        copy.start()
    seqs, props, width = held_ref.shape
    count = seqs * props
    features, channels = kept_ref.shape
    half = features // 2
    copies[0].wait()
    rows = held_ref[...].reshape(count, width)
    copies[1].wait()
    for copy in range(out_ref.shape[0]):
        out_ref[copy, :count] = rows
        out_ref[copy, count:, :channels] = kept_ref[:half]
        out_ref[copy, count:, channels:] = kept_ref[half:]


def contract_last(left, right):
    return lax.dot_general(left, right, (((1,), (1,)), ((), ())), preferred_element_type=F32)


def front_kernel(
    order, picks_from, extra_from, x_ref, gain_from, floor_from, wq_ref, wf_ref, wv_ref, prior_ref,
    out_ref, decay_ref, key_ref, value_ref, picked_ref,
    picks_ref, extra_ref, gain_ref, floor_ref, held_ref, small_sems, sems, pick_sems,
):
    small = [
        pltpu.make_async_copy(source, kept, small_sems.at[at])
        for at, (source, kept) in enumerate(
            (
                (picks_from, picks_ref),
                (gain_from, gain_ref),
                (extra_from, extra_ref),
                (floor_from, floor_ref),
            )
        )
    ]
    for copy in small:
        copy.start()
    seqs, channels, dim = picked_ref.shape
    rows = decay_ref.shape[0]
    blocks, _, width = x_ref.shape
    total = blocks * width
    heads = channels // dim
    props = rows // seqs
    weights = (wq_ref, wf_ref, wv_ref)
    copies = [
        [
            pltpu.make_async_copy(
                weight.at[pl.ds(order[block] * width, width)], held_ref.at[at, block], sems.at[at, block]
            )
            for at, weight in enumerate(weights)
        ]
        for block in range(blocks)
    ]
    for group in copies[:AHEAD]:
        for copy in group:
            copy.start(priority=1)
    small[0].wait()
    picks = [
        pltpu.make_async_copy(
            prior_ref.at[seq, picks_ref[seq] - 1], picked_ref.at[seq], pick_sems.at[seq]
        )
        for seq in range(seqs)
    ]
    for copy in picks:
        copy.start()
    for copy in small[1:]:
        copy.wait()
    square = jnp.zeros((rows, width), F32)
    scaled = []
    for block in range(blocks):
        x = x_ref[block, :rows].astype(F32)
        square = square + x * x
        scaled.append((x * gain_ref[:, order[block] * width : (order[block] + 1) * width]).astype(BF))
    head_of = lax.broadcasted_iota(jnp.int32, (rows, channels), 1) // dim
    row_of = lax.broadcasted_iota(jnp.int32, (rows, channels), 0)
    extra = jnp.zeros((rows, channels), F32)
    for seq in range(seqs):
        for head in range(heads):
            for prop in range(props):
                here = (row_of == seq * props + prop) & (head_of == head)
                extra = jnp.where(here, extra_ref[seq, head, prop], extra)
    boost = jnp.exp(extra)
    sums = [jnp.zeros((rows, channels), F32) for _ in weights]
    for block in range(blocks):
        for at in range(len(weights)):
            copies[block][at].wait()
        for copy in copies[block + AHEAD] if block + AHEAD < blocks else ():
            copy.start(priority=1)
        for at in range(len(weights)):
            sums[at] = sums[at] + jnp.dot(
                scaled[block], held_ref[at, block], preferred_element_type=F32
            )
    scale = lax.rsqrt(jnp.sum(square, axis=1, keepdims=True) / total + 1e-06)
    query_pre, forget_pre, value = ((s * scale).astype(BF).astype(F32) for s in sums)
    query = query_pre / (1.0 + jnp.exp(-query_pre))
    lower = floor_ref[...]
    forget = lower + (1.0 - lower) / (1.0 + jnp.exp(-forget_pre))
    key = 1.0 - forget
    decay = forget * boost
    decay_ref[...] = decay
    key_ref[...] = key
    value_ref[...] = value

    step = row_of % props
    carried = decay
    through = query
    mixed = jnp.zeros((rows, channels), F32)
    for lag in range(props):
        product = (key if lag == 0 else pltpu.roll(key, lag, 0)) * through
        weight = jnp.zeros((rows, channels), F32)
        for head in range(heads):
            weight = jnp.where(
                head_of == head,
                jnp.sum(product[:, head * dim : (head + 1) * dim], axis=1, keepdims=True),
                weight,
            )
        late = value if lag == 0 else pltpu.roll(value, lag, 0)
        mixed = mixed + jnp.where(step >= lag, weight * late, 0.0)
        earlier = decay if lag == 0 else pltpu.roll(decay, lag, 0)
        through = through * earlier
        if lag > 0:
            carried = jnp.where(step >= lag, carried * earlier, carried)
    reach = query * carried
    high = reach.astype(BF)
    low = (reach - high.astype(F32)).astype(BF)
    reach = jnp.concatenate([high, low], axis=0)
    for copy in picks:
        copy.wait()
    seq_of = lax.broadcasted_iota(jnp.int32, (rows, dim), 0) // props
    for head in range(heads):
        span = slice(head * dim, (head + 1) * dim)
        old = jnp.zeros((rows, dim), F32)
        for seq in range(seqs):
            state = picked_ref[seq, span, :]
            state_high = state.astype(BF)
            state_low = (state - state_high.astype(F32)).astype(BF)
            part = contract_last(reach[:, span], state_high)
            part = part[:rows] + part[rows:] + contract_last(high[:, span], state_low)
            old = jnp.where(seq_of == seq, part, old)
        gated = (mixed[:, span] + old).astype(BF)
        for copy in range(out_ref.shape[0]):
            out_ref[copy, :, span] = gated


def states_kernel(picked_ref, decay_ref, key_ref, value_ref, out_ref):
    seqs, props, channels, dim = out_ref.shape
    columns = value_ref[...].T
    for seq in range(seqs):
        for head in range(channels // dim):
            span = slice(head * dim, (head + 1) * dim)
            state = picked_ref[seq, span, :]
            for prop in range(props):
                row = seq * props + prop
                state = (
                    decay_ref[row : row + 1, span] * state
                    + columns[span, row : row + 1] * key_ref[row : row + 1, span]
                )
                out_ref[seq, prop, span, :] = state


def repeat_kernel(rows_ref, out_ref):
    for copy in range(out_ref.shape[0]):
        out_ref[copy] = rows_ref[...]


def product_kernel(order, rows, features, rows_ref, weight_ref, out_ref):
    members, blocks, _, channels = rows_ref.shape
    half = features // 2
    total = jnp.zeros((members * rows, features), F32)
    for block in range(blocks):
        left = jnp.concatenate([rows_ref[order.index(at), block] for at in range(members)], axis=0)
        right = jnp.concatenate(
            [weight_ref[block, rows:, :channels], weight_ref[block, rows:, channels:]], axis=0
        )
        total = total + contract_last(left, right)
    planes = lax.axis_size("zh")
    far = (lax.axis_index("tp") + planes - lax.axis_index("zh")) % planes == planes // 2
    half = members * rows // 2
    out_ref[...] = jnp.where(
        far, jnp.concatenate([total[half:], total[:half]], axis=0), total
    ).astype(BF)


def per_device(
    proposals,
    input_norm_gain,
    query_matrix,
    forget_gate_matrix,
    value_matrix,
    forget_floor_channel,
    proposal_extra_decay,
    prior_proposal_states,
    accepted,
    output_matrix,
):
    seqs, props, width = proposals.shape
    rows = seqs * props
    channels = query_matrix.shape[1]
    dim = prior_proposal_states.shape[3]
    features = output_matrix.shape[1]
    tp = lax.axis_size("tp")
    planes = lax.axis_size("zh")
    slab = lax.axis_size(SLAB)
    shape = jax.ShapeDtypeStruct
    tp_order = led_by(tp, TP_FIRST)
    depth = lax.axis_size("zl")
    slab_order = led_by(slab, ZL_FIRST * lax.axis_size("y") + Y_FIRST)

    pieces = pl.pallas_call(
        spread_kernel,
        out_shape=pltpu.VMEM((tp, rows + features * channels // width, width), BF),
        in_specs=[HBM] * 2,
        out_specs=VM,
        scratch_shapes=[
            pltpu.VMEM(proposals.shape, BF),
            pltpu.VMEM((features, channels), BF),
            pltpu.SemaphoreType.DMA((2,)),
        ],
        compiler_params=grant(4),
    )(in_hbm(proposals), in_hbm(output_matrix.T))
    whole = exchange(pieces, "tp", tp_order)

    blocks = tp
    front = pl.pallas_call(
        lambda *refs: front_kernel(tp_order, *refs),
        out_shape=(pltpu.VMEM((tp, rows, channels), BF),)
        + (shape((rows, channels), F32),) * 3
        + (shape((seqs, channels, dim), F32),),
        in_specs=[HBM] * 2 + [VM] + [HBM] * 6,
        out_specs=[VM] * 5,
        scratch_shapes=[
            pltpu.SMEM(accepted.shape, jnp.int32),
            pltpu.SMEM((seqs, channels // dim, props), F32),
            pltpu.VMEM((1, tp * width), F32),
            pltpu.VMEM((1, channels), F32),
            pltpu.VMEM((3, blocks, width, channels), BF),
            pltpu.SemaphoreType.DMA((4,)),
            pltpu.SemaphoreType.DMA((3, blocks)),
            pltpu.SemaphoreType.DMA((seqs,)),
        ],
        compiler_params=grant(16),
        cost_estimate=pl.CostEstimate(flops=8 << 20, bytes_accessed=6 << 20, transcendentals=0),
    )
    operands = (
        in_hbm(accepted),
        in_hbm(proposal_extra_decay.transpose(0, 2, 1)),
        whole,
        in_hbm(input_norm_gain.reshape(1, -1)),
        in_hbm(forget_floor_channel.reshape(1, -1)),
        *(in_hbm(m) for m in (query_matrix, forget_gate_matrix, value_matrix)),
        in_hbm(prior_proposal_states),
    )
    gated, decay, key, value, picked = front(*operands)
    full = exchange(gated, "tp", tp_order)
    def index(zh, zl, t):
        return (zh * depth + zl) * tp + t

    swap = []
    for zh in range(planes):
        for t in range(tp):
            turn = depth // 2 if (t - zh) % planes == planes // 2 else 0
            for zl in range(depth):
                swap.append((index(zh, zl, t), index(t, (zl + turn) % depth, zh)))
    crossed = lax.ppermute(full, ("zh", "zl", "tp"), swap)

    states = pl.pallas_call(
        states_kernel,
        out_shape=shape((seqs, props, channels, dim), F32),
        in_specs=[VM] * 4,
        out_specs=VM,
        compiler_params=grant(8),
        cost_estimate=pl.CostEstimate(flops=8 << 20, bytes_accessed=1 << 20, transcendentals=0),
    )
    next_states = states(picked, decay, key, value)

    repeated = pl.pallas_call(
        repeat_kernel,
        out_shape=pltpu.VMEM((slab, *crossed.shape), BF),
        in_specs=[VM],
        out_specs=VM,
        compiler_params=grant(4),
    )(crossed)
    gathered = exchange(repeated, SLAB, slab_order)
    result = pl.pallas_call(
        lambda *refs: product_kernel(slab_order, rows, features, *refs),
        out_shape=shape((slab * rows, features), BF),
        in_specs=[VM] * 2,
        out_specs=VM,
        compiler_params=grant(8),
    )(gathered, whole)
    return (result.reshape(slab * seqs, props, features), next_states)


def solution(mesh):
    kv, tp = mesh.shape["kv"], mesh.shape["tp"]
    split = Mesh(mesh.devices.reshape(tp, kv // (4 * tp), 4, tp), ("zh", "zl", "y", "tp"))
    placed = (
        P(KV, None, "tp"),
        P(),
        P(None, "tp"),
        P(None, "tp"),
        P(None, "tp"),
        P("tp"),
        P(KV, None, "tp"),
        P(KV, None, "tp", None),
        P(KV),
        P("tp", KV),
    )
    return jax.shard_map(
        per_device,
        mesh=split,
        in_specs=placed,
        out_specs=(P("tp", None, KV), P(KV, None, "tp", None)),
        check_vma=False,
    )
```

```python
import jax
import jax.numpy as jnp
from jax import lax
from jax.experimental import pallas as pl
from jax.experimental.pallas import tpu as pltpu
from jax.sharding import Mesh
from jax.sharding import PartitionSpec as P

KV = ("zh", "zl", "y")
SLAB = ("zl", "y")
BF = jnp.bfloat16
F32 = jnp.float32
VM = pl.BlockSpec(memory_space=pltpu.VMEM)
ZL_FIRST = 2
Y_FIRST = 3
TP_FIRST = 5
AHEAD = 5
HALF_TURN = (2, 3, 0, 1)
NEAREST = (3, 2, 0, 1)
HBM = pl.BlockSpec(memory_space=pltpu.HBM)


def exchange(pieces, axes, *orders):
    return lax.all_to_all(
        pieces, axes, 0, 0, tiled=True, axis_index_groups=[list(order) for order in orders]
    )


def first_row():
    at = [lax.axis_index(axis) for axis in KV]
    return at[0] + at[1] + at[2] == 0


def leads_turned(order):
    first = first_row()
    return [jnp.where(first, order[1], order[0]), jnp.where(first, order[0], order[1]), *order[2:]]


def led_by(count, first):
    return [first] + [at for at in range(count) if at != first]


def grant(mebibytes):
    return pltpu.CompilerParams(vmem_limit_bytes=mebibytes << 20)


def in_hbm(array):
    return pltpu.with_memory_space_constraint(array, pltpu.HBM)


def spread_kernel(rows_ref, weight_ref, out_ref, held_ref, kept_ref, sems):
    copies = [
        pltpu.make_async_copy(rows_ref, held_ref, sems.at[0]),
        pltpu.make_async_copy(weight_ref, kept_ref, sems.at[1]),
    ]
    for copy in copies:
        copy.start()
    seqs, props, width = held_ref.shape
    count = seqs * props
    features, channels = kept_ref.shape
    half = features // 2
    copies[0].wait()
    rows = held_ref[...].reshape(count, width)
    copies[1].wait()
    for copy in range(out_ref.shape[0]):
        out_ref[copy, :count] = rows
        out_ref[copy, count:, :channels] = kept_ref[:half]
        out_ref[copy, count:, channels:] = kept_ref[half:]


def contract_last(left, right):
    return lax.dot_general(left, right, (((1,), (1,)), ((), ())), preferred_element_type=F32)


def front_kernel(
    order, picks_from, extra_from, x_ref, gain_from, floor_from, wq_ref, wf_ref, wv_ref, prior_ref,
    out_ref, decay_ref, key_ref, value_ref, picked_ref,
    picks_ref, extra_ref, gain_ref, floor_ref, held_ref, small_sems, sems, pick_sems,
):
    small = [
        pltpu.make_async_copy(source, kept, small_sems.at[at])
        for at, (source, kept) in enumerate(
            (
                (picks_from, picks_ref),
                (gain_from, gain_ref),
                (extra_from, extra_ref),
                (floor_from, floor_ref),
            )
        )
    ]
    for copy in small:
        copy.start()
    seqs, channels, dim = picked_ref.shape
    rows = decay_ref.shape[0]
    blocks, _, width = x_ref.shape
    total = blocks * width
    heads = channels // dim
    props = rows // seqs
    weights = (wq_ref, wf_ref, wv_ref)
    spans = [pl.ds(pl.multiple_of(at * width, width), width) for at in leads_turned(order)]
    copies = [
        [
            pltpu.make_async_copy(
                weight.at[spans[block]], held_ref.at[at, block], sems.at[at, block]
            )
            for at, weight in enumerate(weights)
        ]
        for block in range(blocks)
    ]
    for group in copies[:AHEAD]:
        for copy in group:
            copy.start(priority=1)
    small[0].wait()
    picks = [
        pltpu.make_async_copy(
            prior_ref.at[seq, picks_ref[seq] - 1], picked_ref.at[seq], pick_sems.at[seq]
        )
        for seq in range(seqs)
    ]
    for copy in picks:
        copy.start()
    for copy in small[1:]:
        copy.wait()
    square = jnp.zeros((rows, width), F32)
    scaled = []
    for block in range(blocks):
        x = x_ref[block, :rows].astype(F32)
        square = square + x * x
        scaled.append((x * gain_ref[:, spans[block]]).astype(BF))
    head_of = lax.broadcasted_iota(jnp.int32, (rows, channels), 1) // dim
    row_of = lax.broadcasted_iota(jnp.int32, (rows, channels), 0)
    extra = jnp.zeros((rows, channels), F32)
    for seq in range(seqs):
        for head in range(heads):
            for prop in range(props):
                here = (row_of == seq * props + prop) & (head_of == head)
                extra = jnp.where(here, extra_ref[seq, head, prop], extra)
    boost = jnp.exp(extra)
    sums = [jnp.zeros((rows, channels), F32) for _ in weights]
    for block in range(blocks):
        for at in range(len(weights)):
            copies[block][at].wait()
        for copy in copies[block + AHEAD] if block + AHEAD < blocks else ():
            copy.start(priority=1)
        for at in range(len(weights)):
            sums[at] = sums[at] + jnp.dot(
                scaled[block], held_ref[at, block], preferred_element_type=F32
            )
    scale = lax.rsqrt(jnp.sum(square, axis=1, keepdims=True) / total + 1e-06)
    query_pre, forget_pre, value = ((s * scale).astype(BF).astype(F32) for s in sums)
    query = query_pre / (1.0 + jnp.exp(-query_pre))
    lower = floor_ref[...]
    forget = lower + (1.0 - lower) / (1.0 + jnp.exp(-forget_pre))
    key = 1.0 - forget
    decay = forget * boost
    decay_ref[...] = decay
    key_ref[...] = key
    value_ref[...] = value

    step = row_of % props
    carried = decay
    through = query
    mixed = jnp.zeros((rows, channels), F32)
    for lag in range(props):
        product = (key if lag == 0 else pltpu.roll(key, lag, 0)) * through
        weight = jnp.zeros((rows, channels), F32)
        for head in range(heads):
            weight = jnp.where(
                head_of == head,
                jnp.sum(product[:, head * dim : (head + 1) * dim], axis=1, keepdims=True),
                weight,
            )
        late = value if lag == 0 else pltpu.roll(value, lag, 0)
        mixed = mixed + jnp.where(step >= lag, weight * late, 0.0)
        earlier = decay if lag == 0 else pltpu.roll(decay, lag, 0)
        through = through * earlier
        if lag > 0:
            carried = jnp.where(step >= lag, carried * earlier, carried)
    reach = query * carried
    high = reach.astype(BF)
    low = (reach - high.astype(F32)).astype(BF)
    reach = jnp.concatenate([high, low], axis=0)
    for copy in picks:
        copy.wait()
    seq_of = lax.broadcasted_iota(jnp.int32, (rows, dim), 0) // props
    for head in range(heads):
        span = slice(head * dim, (head + 1) * dim)
        old = jnp.zeros((rows, dim), F32)
        for seq in range(seqs):
            state = picked_ref[seq, span, :]
            state_high = state.astype(BF)
            state_low = (state - state_high.astype(F32)).astype(BF)
            part = contract_last(reach[:, span], state_high)
            part = part[:rows] + part[rows:] + contract_last(high[:, span], state_low)
            old = jnp.where(seq_of == seq, part, old)
        gated = (mixed[:, span] + old).astype(BF)
        for copy in range(out_ref.shape[0]):
            out_ref[copy, :, span] = gated


def states_kernel(picked_ref, decay_ref, key_ref, value_ref, out_ref):
    seqs, props, channels, dim = out_ref.shape
    columns = value_ref[...].T
    for seq in range(seqs):
        for head in range(channels // dim):
            span = slice(head * dim, (head + 1) * dim)
            state = picked_ref[seq, span, :]
            for prop in range(props):
                row = seq * props + prop
                state = (
                    decay_ref[row : row + 1, span] * state
                    + columns[span, row : row + 1] * key_ref[row : row + 1, span]
                )
                out_ref[seq, prop, span, :] = state


def plane_for(zh, to, zl, y, planes):
    if (to - zh) % planes != planes // 2:
        return zl
    table = NEAREST if y == 0 else HALF_TURN
    return table[zl] if zh < to else table.index(zl)


def is_far():
    planes = lax.axis_size("zh")
    return (lax.axis_index("tp") + planes - lax.axis_index("zh")) % planes == planes // 2


def repeat_kernel(rows_ref, out_ref):
    source = jnp.where(is_far(), NEAREST[0], 0)
    turned = (lax.axis_index("tp") + lax.axis_index("y") == 0) & (lax.axis_index("zl") == source)
    first = jnp.where(turned, 1, 0)
    for copy in range(out_ref.shape[0]):
        out_ref[copy, 0] = rows_ref[first]
        out_ref[copy, 1] = rows_ref[1 - first]
        out_ref[copy, 2:] = rows_ref[2:]


def product_kernel(order, rows, features, rows_ref, weight_ref, out_ref):
    members, blocks, _, channels = rows_ref.shape
    total = jnp.zeros((members * rows, features), F32)
    sources = leads_turned(list(range(blocks)))
    for block in range(blocks):
        left = jnp.concatenate([rows_ref[order.index(at), block] for at in range(members)], axis=0)
        right = jnp.concatenate(
            [
                weight_ref[sources[block], rows:, :channels],
                weight_ref[sources[block], rows:, channels:],
            ],
            axis=0,
        )
        total = total + contract_last(left, right)
    planes, depth, side = (lax.axis_size(axis) for axis in KV)

    def placed(zh, to):
        at = [
            plane_for(zh, to, zl, y, planes) * side + y for zl in range(depth) for y in range(side)
        ]
        return jnp.concatenate([total[member * rows : (member + 1) * rows] for member in at], axis=0)

    upper = lax.axis_index("zh") >= planes // 2
    far = jnp.where(upper, placed(0, planes // 2), placed(planes // 2, 0))
    out_ref[...] = jnp.where(is_far(), far, total).astype(BF)


def per_device(
    proposals,
    input_norm_gain,
    query_matrix,
    forget_gate_matrix,
    value_matrix,
    forget_floor_channel,
    proposal_extra_decay,
    prior_proposal_states,
    accepted,
    output_matrix,
):
    seqs, props, width = proposals.shape
    rows = seqs * props
    channels = query_matrix.shape[1]
    dim = prior_proposal_states.shape[3]
    features = output_matrix.shape[1]
    tp = lax.axis_size("tp")
    planes = lax.axis_size("zh")
    slab = lax.axis_size(SLAB)
    shape = jax.ShapeDtypeStruct
    tp_order = led_by(tp, TP_FIRST)
    depth = lax.axis_size("zl")
    slab_order = led_by(slab, ZL_FIRST * lax.axis_size("y") + Y_FIRST)

    pieces = pl.pallas_call(
        spread_kernel,
        out_shape=pltpu.VMEM((tp, rows + features * channels // width, width), BF),
        in_specs=[HBM] * 2,
        out_specs=VM,
        scratch_shapes=[
            pltpu.VMEM(proposals.shape, BF),
            pltpu.VMEM((features, channels), BF),
            pltpu.SemaphoreType.DMA((2,)),
        ],
        compiler_params=grant(4),
    )(in_hbm(proposals), in_hbm(output_matrix.T))
    turned = [tp_order[1], tp_order[0], *tp_order[2:]]
    row_orders = [
        [row * tp + t for t in (turned if row == 0 else tp_order)]
        for row in range(planes * slab)
    ]
    whole = exchange(pieces, (*KV, "tp"), *row_orders)

    blocks = tp
    front = pl.pallas_call(
        lambda *refs: front_kernel(tp_order, *refs),
        out_shape=(pltpu.VMEM((tp, rows, channels), BF),)
        + (shape((rows, channels), F32),) * 3
        + (shape((seqs, channels, dim), F32),),
        in_specs=[HBM] * 2 + [VM] + [HBM] * 6,
        out_specs=[VM] * 5,
        scratch_shapes=[
            pltpu.SMEM(accepted.shape, jnp.int32),
            pltpu.SMEM((seqs, channels // dim, props), F32),
            pltpu.VMEM((1, tp * width), F32),
            pltpu.VMEM((1, channels), F32),
            pltpu.VMEM((3, blocks, width, channels), BF),
            pltpu.SemaphoreType.DMA((4,)),
            pltpu.SemaphoreType.DMA((3, blocks)),
            pltpu.SemaphoreType.DMA((seqs,)),
        ],
        compiler_params=grant(16),
        cost_estimate=pl.CostEstimate(flops=8 << 20, bytes_accessed=6 << 20, transcendentals=0),
    )
    operands = (
        in_hbm(accepted),
        in_hbm(proposal_extra_decay.transpose(0, 2, 1)),
        whole,
        in_hbm(input_norm_gain.reshape(1, -1)),
        in_hbm(forget_floor_channel.reshape(1, -1)),
        *(in_hbm(m) for m in (query_matrix, forget_gate_matrix, value_matrix)),
        in_hbm(prior_proposal_states),
    )
    gated, decay, key, value, picked = front(*operands)
    full = exchange(gated, (*KV, "tp"), *row_orders)
    side = lax.axis_size("y")

    def index(zh, zl, y, t):
        return ((zh * depth + zl) * side + y) * tp + t

    swap = [
        (index(zh, zl, y, t), index(t, plane_for(zh, t, zl, y, planes), y, zh))
        for zh in range(planes)
        for zl in range(depth)
        for y in range(side)
        for t in range(tp)
    ]
    crossed = lax.ppermute(full, (*KV, "tp"), swap)

    states = pl.pallas_call(
        states_kernel,
        out_shape=shape((seqs, props, channels, dim), F32),
        in_specs=[VM] * 4,
        out_specs=VM,
        compiler_params=grant(8),
        cost_estimate=pl.CostEstimate(flops=8 << 20, bytes_accessed=1 << 20, transcendentals=0),
    )
    next_states = states(picked, decay, key, value)

    repeated = pl.pallas_call(
        repeat_kernel,
        out_shape=pltpu.VMEM((slab, *crossed.shape), BF),
        in_specs=[VM],
        out_specs=VM,
        compiler_params=grant(4),
    )(crossed)
    gathered = exchange(repeated, SLAB, slab_order)
    result = pl.pallas_call(
        lambda *refs: product_kernel(slab_order, rows, features, *refs),
        out_shape=shape((slab * rows, features), BF),
        in_specs=[VM] * 2,
        out_specs=VM,
        compiler_params=grant(8),
    )(gathered, whole)
    return (result.reshape(slab * seqs, props, features), next_states)


def solution(mesh):
    kv, tp = mesh.shape["kv"], mesh.shape["tp"]
    split = Mesh(mesh.devices.reshape(tp, kv // (4 * tp), 4, tp), ("zh", "zl", "y", "tp"))
    placed = (
        P(KV, None, "tp"),
        P(),
        P(None, "tp"),
        P(None, "tp"),
        P(None, "tp"),
        P("tp"),
        P(KV, None, "tp"),
        P(KV, None, "tp", None),
        P(KV),
        P("tp", KV),
    )
    return jax.shard_map(
        per_device,
        mesh=split,
        in_specs=placed,
        out_specs=(P("tp", None, KV), P(KV, None, "tp", None)),
        check_vma=False,
    )
```
